32 devices in a mesh: sp: 16 (over z, y, x), tp: 2 (over core).
Axes of the slice: x: 2, y: 2, z: 4, core: 2. Of those that a mesh axis runs over, the one named last changes fastest.
Arguments:
- conv_in: bfloat16 [4096, 1024], P('sp', 'tp'), may hold values from -6 to 6
- gate_outer: bfloat16 [4096, 1024], P('sp', 'tp'), may hold values from -6 to 6
- gate_inner: bfloat16 [4096, 1024], P('sp', 'tp'), may hold values from -6 to 6
- tap_weights: float32 [3, 1024], P(None, 'tp'), may hold values from -3 to 3
- doc_ids: int32 [4096], P('sp'), may hold values from 0 to 7, never falling along the last dimension, each value on 1 to 1024 neighbouring positions
- w_proj: bfloat16 [1024, 2048], replicated, may hold values from -0.1875 to 0.1875
- stream: bfloat16 [4096, 2048], P(('sp', 'tp')), may hold values from -6 to 6
- norm_gain: float32 [2048], replicated, may hold values from 0.1 to 1.9
- routes: int32 [4096, 4], P(('sp', 'tp')), may hold values from 0 to 31, all different within a row; in each aligned block of 128 rows (0 to 127, 128 to 255, ...) at most 32 rows name the same one
- route_weights: float32 [4096, 4], P(('sp', 'tp')), may hold values from 0.1 to 1
- w_gate: bfloat16 [32, 2048, 768], P(('sp', 'tp')), may hold values from -0.5 to 0.5
- w_up: bfloat16 [32, 2048, 768], P(('sp', 'tp')), may hold values from -0.5 to 0.5
- w_down: bfloat16 [32, 768, 2048], P(('sp', 'tp')), may hold values from -0.0546875 to 0.0546875
Outputs:
- layer_out: bfloat16 [4096, 2048], P(('sp', 'tp'))
The draws below stay inside these ranges and needn't reach their ends.
Inputs may be any that keep to these rules, and one draw needn't show every extreme that they name: `doc_ids`: document numbers never fall along the sequence; a document covers at most 1024 positions. `routes`: a token names 4 different experts; among the rows of one device (aligned blocks of 128 tokens) no expert is named more than 32 times, a bound that some block reaches.
All inputs are finite; a program needn't handle non-finite values.
Results may differ from the reference program's by a relative error of at most 0.0071.
Values may be sent and summed in bfloat16 or wider, within the bound.
No kernel may reach another device: no remote copies, remote signals or barrier semaphores. Data moves between devices by JAX's collectives and lax.ppermute only.
A program may use at most 128 MiB of HBM per device.

```python
import math
import jax
import jax.numpy as jnp
import numpy as np
from jax import lax

D = 2048
CW = 1024
FF = 768
TOPK = 4
TAPS = 3
TOK_DEV = 256
TOKENS = 4096
EXPERTS = 32
BLOCK = 128
CAP = 32
DOCS = 8
DOC_MOST = 1024
N_TP = 2


def block_scale(own_key, dims, split, low, top_value):
    def one(position, blocks):
        draws = jax.random.uniform(jax.random.fold_in(jax.random.fold_in(own_key, 6), position), (blocks,), jnp.float32, low / len(split), top_value / len(split))
        return jnp.repeat(jnp.exp(draws), dims[position] // blocks).reshape((-1,) + (1,) * (len(dims) - position - 1))

    factor_of = one(*split[0])
    for cut in split[1:]:
        factor_of = factor_of * one(*cut)
    return factor_of


def split_up(number_of, total, most, skew):
    portions = [(1 << 20) // math.isqrt(rank ** skew) + 1 for rank in range(2, number_of + 1)]
    rest, holding = total - most - (number_of - 1), [1] * (number_of - 1)
    while rest > 0:
        movable = [i for i in range(number_of - 1) if holding[i] < most]
        whole, remaining = sum([portions[i] for i in movable]), rest
        for i in movable:
            extra = min(most - holding[i], max(1, remaining * portions[i] // whole), rest)
            holding[i] = holding[i] + extra
            rest = rest - extra
    return np.array([most] + holding)


def ragged(own_key, count, total, bound, lean):
    if count == 2:
        one = jax.random.randint(own_key, (), max(1, total - bound), min(bound, total - 1) + 1)
        return jnp.stack([one, total - one])
    sizes = jnp.asarray(split_up(count, total, bound, lean), jnp.int32)
    twos = (count - 1) // 2
    giver, taker = sizes[1:1 + 2 * twos:2], sizes[2:2 + 2 * twos:2]
    margin = jnp.minimum(giver - 1, bound - taker)
    passed = jax.random.randint(jax.random.fold_in(own_key, 1), (twos,), 0, 1 << 20) % (margin + 1)
    sizes = sizes.at[1:1 + 2 * twos:2].set(giver - passed).at[2:2 + 2 * twos:2].set(taker + passed)
    return sizes[jax.random.permutation(jax.random.fold_in(own_key, 2), count)]


def shared_out(own_key, own, number, rows, amount, top, most, slope):
    ranking = jax.random.permutation(own_key, amount)
    heavy_load, common = portions_of(amount, rows * top, most, slope, True), portions_of(amount, rows * top, most, slope, False)
    places = jnp.arange(amount)

    def named(lengths, offset_by):
        used = int((lengths > 0).sum())
        fixed = max(1, used // 4)
        moved = fixed + (places - fixed + offset_by * (used - fixed)) % max(1, amount - fixed)
        return jnp.zeros((amount,), jnp.int32).at[ranking[jnp.where(places < fixed, places, moved)]].set(jnp.asarray(lengths, jnp.int32))

    lengths = jnp.where(number % 4 == 0, named(heavy_load, number // 4), named(common, number - number // 4 - 1))
    mixed = jax.random.permutation(jax.random.fold_in(own, 3), amount)
    donor, sink = mixed[0:amount // 2 * 2:2], mixed[1:amount // 2 * 2:2]
    room = jnp.minimum(lengths[donor] - 1, most - lengths[sink]) // 2
    room = jnp.where((donor == ranking[0]) | (sink == ranking[0]) | (lengths[sink] == 0), 0, jnp.maximum(room, 0))
    moved = jax.random.randint(jax.random.fold_in(own, 4), (amount // 2,), 0, 1 << 20) % (room + 1)
    lengths = lengths.at[donor].add(-moved).at[sink].add(moved)
    members = jnp.searchsorted(jnp.cumsum(lengths), jnp.arange(rows * top), side="right").astype(jnp.int32)
    table = members.reshape(top, rows).T
    table = table[jax.random.permutation(jax.random.fold_in(own, 1), rows)]
    offset_by = jax.random.randint(jax.random.fold_in(own, 2), (rows, 1), 0, top)
    return jnp.take_along_axis(table, (jnp.arange(top)[None, :] + offset_by) % top, axis=1)


def portions_of(amount, total, most, skew, full):
    portions = [(1 << 20) // math.isqrt(grade ** skew) + 1 for grade in range(1, amount + 1)]
    largest = most if full else min(most, max(-(-total // amount), total * portions[0] // sum(portions)))
    least = 1 if total - largest >= amount - 1 else 0
    holding, rest = [largest] + [least] * (amount - 1), total - largest - least * (amount - 1)
    while rest > 0:
        free = [i for i in range(1, amount) if holding[i] < largest] or [i for i in range(1, amount) if holding[i] < most]
        pool, remaining = sum([portions[i] for i in free]), rest
        for i in free:
            more = min(most - holding[i], max(1, remaining * portions[i] // pool), rest)
            holding[i] = holding[i] + more
            rest = rest - more
    return np.array(holding)


def noise(rng, shape, width, limit, pieces=(), held_as=jnp.bfloat16):
    entries = width * jax.random.normal(rng, shape, jnp.float32)
    if pieces:
        entries = entries * block_scale(rng, shape, pieces, -0.22, 0.18)
    return jnp.clip(entries, -limit, limit).astype(held_as)


def setup_inputs(seed: int = 0) -> dict:
    arg_keys = jax.random.split(jax.random.key(seed), 14)
    conv_in = noise(arg_keys[0], (TOKENS, CW), 1.0, 6.0, ((0, 16), (1, 2)))
    gate_outer = noise(arg_keys[1], (TOKENS, CW), 1.0, 6.0, ((0, 16), (1, 2)))
    gate_inner = noise(arg_keys[2], (TOKENS, CW), 1.0, 6.0, ((0, 16), (1, 2)))
    tap_weights = noise(arg_keys[3], (TAPS, CW), 0.6, 3.0, ((1, 2),), jnp.float32)
    doc_ids = jnp.searchsorted(jnp.cumsum(ragged(arg_keys[4], DOCS, TOKENS, DOC_MOST, 0)), jnp.arange(TOKENS), side="right").astype(jnp.int32)
    w_proj = noise(arg_keys[5], (CW, D), CW ** -0.5, 0.1875)
    stream = noise(arg_keys[6], (TOKENS, D), 1.0, 6.0, ((0, 32),))
    norm_gain = jnp.clip(1.0 + 0.18 * jax.random.normal(arg_keys[7], (D,), jnp.float32), 0.1, 1.9)
    routes_keys = jax.random.split(jax.random.fold_in(arg_keys[8], 1), TOKENS // BLOCK)
    routes_turns = jax.random.permutation(jax.random.fold_in(arg_keys[8], 3), TOKENS // BLOCK)
    routes = jax.vmap(lambda own, number: shared_out(jax.random.fold_in(arg_keys[8], 2), own, number, BLOCK, EXPERTS, TOPK, CAP, 1))(routes_keys, routes_turns).reshape((TOKENS, TOPK))
    route_weights = jnp.clip(jnp.exp(math.log(1.0) - 2.3025851 * jax.random.uniform(arg_keys[9], (TOKENS, TOPK), jnp.float32) ** block_scale(arg_keys[9], (TOKENS, TOPK), ((0, 32),), -0.2, 0.2)), 0.1, 1.0)
    w_gate = noise(arg_keys[10], (EXPERTS, D, FF), (D // 16) ** -0.5, 0.5, ((0, 32),))
    w_up = noise(arg_keys[11], (EXPERTS, D, FF), (D // 16) ** -0.5, 0.5, ((0, 32),))
    w_down = noise(arg_keys[12], (EXPERTS, FF, D), (16 * FF) ** -0.5, 0.0546875, ((0, 32),))
    return dict(conv_in=conv_in, gate_outer=gate_outer, gate_inner=gate_inner, tap_weights=tap_weights, doc_ids=doc_ids, w_proj=w_proj, stream=stream, norm_gain=norm_gain, routes=routes, route_weights=route_weights, w_gate=w_gate, w_up=w_up, w_down=w_down)


def expert_rows(rows, wg, wu, wd):
    gate = jnp.minimum(jnp.dot(rows, wg, preferred_element_type=jnp.float32), 7.0)
    upper = jnp.clip(jnp.dot(rows, wu, preferred_element_type=jnp.float32), -7.0, 7.0)
    act = ((upper + 1.0) * gate * jax.nn.sigmoid(1.702 * gate)).astype(jnp.bfloat16)
    return jnp.dot(act, wd, preferred_element_type=jnp.float32).astype(jnp.bfloat16)

def reference(conv_in, gate_outer, gate_inner, tap_weights, doc_ids, w_proj, stream, norm_gain, routes, route_weights, w_gate, w_up, w_down):
    product = gate_inner.astype(jnp.float32) * conv_in.astype(jnp.float32)
    same = (doc_ids[1:] == doc_ids[:-1]).astype(jnp.float32)
    zero_row = jnp.zeros((1, product.shape[1]), jnp.float32)
    before = jnp.concatenate([zero_row, product[:-1] * same[:, None]], axis=0)
    after = jnp.concatenate([product[1:] * same[:, None], zero_row], axis=0)
    conv = tap_weights[0] * before + tap_weights[1] * product + tap_weights[2] * after
    mixed = (gate_outer.astype(jnp.float32) * conv).astype(jnp.bfloat16)
    hidden = stream.astype(jnp.float32) + jnp.dot(mixed, w_proj, preferred_element_type=jnp.float32)
    scale = lax.rsqrt(lax.optimization_barrier(jnp.mean(hidden * hidden, axis=-1, keepdims=True)) + 1e-05)
    normed = (hidden * scale * norm_gain).astype(jnp.bfloat16)
    block = TOK_DEV // N_TP
    nblocks = TOKENS // block
    slots = nblocks * CAP
    chosen = routes.reshape(nblocks, block * TOPK)
    onehot = (chosen[:, :, None] == jnp.arange(EXPERTS, dtype=jnp.int32)[None, None, :]).astype(jnp.int32)
    ranks = lax.optimization_barrier(jnp.sum(jnp.cumsum(onehot, axis=1) * onehot, axis=-1)) - 1
    block_ids = jnp.arange(nblocks, dtype=jnp.int32)[:, None]
    places = (chosen * slots + block_ids * CAP + ranks).reshape(-1).astype(jnp.int32)
    owners = (block_ids * block + (jnp.arange(block * TOPK, dtype=jnp.int32) // TOPK)[None, :]).reshape(-1)
    table = jnp.full((EXPERTS * slots,), TOKENS, jnp.int32).at[places].set(owners).reshape(EXPERTS, slots)
    weights = jnp.zeros((EXPERTS * slots,), jnp.float32).at[places].set(route_weights.reshape(-1)).reshape(EXPERTS, slots)
    padded = jnp.concatenate([normed, jnp.zeros((1, normed.shape[1]), jnp.bfloat16)], axis=0)

    def one_expert(total, items):
        owner_ids, owner_weights, wg, wu, wd = items
        result = expert_rows(padded[owner_ids], wg, wu, wd)
        total = total.at[owner_ids].add(result.astype(jnp.float32) * owner_weights[:, None])
        return (total, None)
    start = jnp.zeros((TOKENS + 1, normed.shape[1]), jnp.float32)
    total, _ = lax.scan(one_expert, start, (table, weights, w_gate, w_up, w_down))
    return (hidden + total[:TOKENS]).astype(jnp.bfloat16)
```

```python
import math

import jax
import jax.numpy as jnp
from jax import lax
from jax.sharding import Mesh, PartitionSpec as P


SEQ = ("z", "p")
ALL = ("z", "p", "tp")
PLANE = ("p", "tp")


def halo_rows(product, doc_float):
    size = lax.axis_size(SEQ)
    up = [(i, i + 1) for i in range(size - 1)]
    down = [(j, i) for i, j in up]
    tail = lambda d: jnp.broadcast_to(d.reshape(1, 1), (1, 128))
    last = jnp.concatenate([product[-1:], tail(doc_float[-1])], axis=1)
    first = jnp.concatenate([product[:1], tail(doc_float[0])], axis=1)
    return lax.ppermute(last, SEQ, up), lax.ppermute(first, SEQ, down)


def expert_rows(rows, wg, wu, wd):
    gate = jnp.minimum(jnp.dot(rows, wg, preferred_element_type=jnp.float32), 7.0)
    upper = jnp.clip(jnp.dot(rows, wu, preferred_element_type=jnp.float32), -7.0, 7.0)
    act = ((upper + 1.0) * gate * jax.nn.sigmoid(1.702 * gate)).astype(jnp.bfloat16)
    return jnp.dot(act, wd, preferred_element_type=jnp.float32).astype(jnp.bfloat16)


def slot_maps(table, topk, first_expert, n_plane, capacity):
    block = table.shape[1]
    experts = (first_expert + jnp.arange(n_plane, dtype=jnp.int32)).astype(jnp.float32)
    named = jnp.zeros((n_plane, block), jnp.float32)
    weight = jnp.zeros((n_plane, block), jnp.float32)
    for k in range(topk):
        hit = table[k][None, :] == experts[:, None]
        named = named + hit.astype(jnp.float32)
        weight = weight + jnp.where(hit, table[topk + k][None, :], 0.0)
    order = jnp.arange(block, dtype=jnp.int32)
    earlier = (order[:, None] < order[None, :]).astype(jnp.bfloat16)
    rank = jnp.dot(named.astype(jnp.bfloat16), earlier, preferred_element_type=jnp.float32)
    rank = jnp.where(named > 0.0, rank, -1.0)
    slots = jnp.arange(capacity, dtype=jnp.int32).astype(jnp.float32)
    onehot = rank[:, None, :] == slots[None, :, None]
    select = onehot.astype(jnp.bfloat16).reshape(n_plane * capacity, block)
    scaled = jnp.where(onehot, weight[:, None, :], 0.0).reshape(n_plane * capacity, block)
    high = scaled.astype(jnp.bfloat16)
    low = (scaled - high.astype(jnp.float32)).astype(jnp.bfloat16)
    return select, high, low


def per_device(
    conv_in,
    gate_outer,
    gate_inner,
    tap_weights,
    doc_ids,
    w_proj,
    stream,
    norm_gain,
    routes,
    route_weights,
    w_gate,
    w_up,
    w_down,
):
    n_z = lax.axis_size("z")
    n_plane = lax.axis_size(PLANE)
    n_core = lax.axis_size("tp")
    tok_dev = conv_in.shape[0]
    width = w_proj.shape[1]
    topk = routes.shape[1]
    block = tok_dev // n_core
    n_expert = n_z * n_plane
    capacity = max(2, 2 * tok_dev * topk // (n_core * n_expert))

    def along_z(x, shift):
        return lax.ppermute(x, "z", [(i, (i + shift) % n_z) for i in range(n_z)])

    doc_float = doc_ids.astype(jnp.float32)
    product = gate_inner.astype(jnp.float32) * conv_in.astype(jnp.float32)
    before, after = halo_rows(product, doc_float)
    table = jnp.concatenate([routes.astype(jnp.float32).T, route_weights.T], axis=0)
    tables = [table] + [along_z(table, s) for s in range(1, n_z)]

    half = product.shape[1]
    wide_prod = jnp.concatenate([before[:, :half], product, after[:, :half]], axis=0)
    wide_docs = jnp.concatenate([before[0, half : half + 1], doc_float, after[0, half : half + 1]])
    same_before = (wide_docs[1:-1] == wide_docs[:-2]).astype(jnp.float32)
    same_after = (wide_docs[1:-1] == wide_docs[2:]).astype(jnp.float32)
    conv = (
        tap_weights[0] * wide_prod[:-2] * same_before[:, None]
        + tap_weights[1] * product
        + tap_weights[2] * wide_prod[2:] * same_after[:, None]
    )
    mixed = (gate_outer.astype(jnp.float32) * conv).astype(jnp.bfloat16)
    regrouped = lax.all_to_all(mixed, "tp", split_axis=0, concat_axis=1, tiled=True)
    projected = jnp.dot(regrouped, w_proj, preferred_element_type=jnp.float32)
    hidden = stream.astype(jnp.float32) + projected
    scale = lax.rsqrt(jnp.mean(hidden * hidden, axis=-1, keepdims=True) + 1e-05)
    normed = (hidden * scale * norm_gain).astype(jnp.bfloat16)

    first_expert = lax.axis_index("z").astype(jnp.int32) * n_plane
    blocks = [normed] + [along_z(normed, s) for s in range(1, n_z)]
    total = hidden
    partials = []
    for s in range(n_z):
        select, high, low = slot_maps(tables[s], topk, first_expert, n_plane, capacity)
        outgoing = jnp.dot(select, blocks[s], preferred_element_type=jnp.float32).astype(jnp.bfloat16)
        arrived = lax.all_to_all(outgoing, PLANE, split_axis=0, concat_axis=0, tiled=True)
        results = expert_rows(arrived, w_gate[0], w_up[0], w_down[0])
        returned = lax.all_to_all(results, PLANE, split_axis=0, concat_axis=0, tiled=True)
        pick = lambda m: lax.dot_general(
            m, returned, (((0,), (0,)), ((), ())), preferred_element_type=jnp.float32
        )
        partial = pick(high) + pick(low)
        if s:
            partial = along_z(partial.astype(jnp.bfloat16), -s).astype(jnp.float32)
        partials.append(partial)
    for partial in partials:
        total = total + partial
    return total.astype(jnp.bfloat16)


def solution(mesh):
    n_seq, n_core = mesh.shape["sp"], mesh.shape["tp"]
    n_z = max(d for d in range(1, math.isqrt(n_seq) + 1) if n_seq % d == 0)
    inner = Mesh(mesh.devices.reshape(n_z, n_seq // n_z, n_core), ALL)
    in_specs = (
        P(SEQ, "tp"),
        P(SEQ, "tp"),
        P(SEQ, "tp"),
        P(None, "tp"),
        P(SEQ),
        P(),
        P(ALL, None),
        P(),
        P(ALL, None),
        P(ALL, None),
        P(ALL, None, None),
        P(ALL, None, None),
        P(ALL, None, None),
    )
    return jax.shard_map(
        per_device, mesh=inner, in_specs=in_specs, out_specs=P(ALL, None), check_vma=False
    )
```
